32 devices in a mesh: ra: 4 (over y, x), cb: 8 (over z, core).
Axes of the slice: x: 2, y: 2, z: 4, core: 2. Of those that a mesh axis runs over, the one named last changes fastest.
Arguments:
- tokens: bfloat16 [2048, 2048], P('cb', 'ra'), may hold values from -40 to 40
- gain_first: float32 [2048], replicated, may hold values from 0.1 to 1.9
- gate_first: float32 [2048, 5632], P('cb', 'ra'), may hold values from -0.125 to 0.125
- gate_first_scale: float32 [5632], P('ra'), may hold values from 0.5 to 2
- up_first: float32 [2048, 5632], P('cb', 'ra'), may hold values from -0.125 to 0.125
- up_first_scale: float32 [5632], P('ra'), may hold values from 0.5 to 2
- down_first: float32 [5632, 2048], P('ra', 'cb'), may hold values from -0.078125 to 0.078125
- down_first_scale: float32 [2048], replicated, may hold values from 0.5 to 2
- gain_second: float32 [2048], replicated, may hold values from 0.1 to 1.9
- gate_second: float32 [2048, 5632], P('cb', 'ra'), may hold values from -0.125 to 0.125
- gate_second_scale: float32 [5632], P('ra'), may hold values from 0.5 to 2
- up_second: float32 [2048, 5632], P('cb', 'ra'), may hold values from -0.125 to 0.125
- up_second_scale: float32 [5632], P('ra'), may hold values from 0.5 to 2
- down_second: float32 [5632, 2048], P('ra', 'cb'), may hold values from -0.078125 to 0.078125
- down_second_scale: float32 [2048], replicated, may hold values from 0.5 to 2
- gain_last: float32 [2048], replicated, may hold values from 0.1 to 1.9
Outputs:
- mixed: bfloat16 [2048, 2048], P('cb', 'ra')
The draws below stay inside these ranges and needn't reach their ends.
All inputs are finite; a program needn't handle non-finite values.
Results may differ from the reference program's by a relative error of at most 0.025.
Values may be sent and summed in bfloat16 or wider, within the bound.
A program may use at most 64 MiB of HBM per device.

```python
import math
import jax
import jax.numpy as jnp
from jax import lax

D = 2048
FF = 5632
TOK = 2048


def draw_tokens(key, part):
    first_key = jax.random.fold_in(key, 11)
    second_key = jax.random.fold_in(key, 12)
    column = jnp.arange(D, dtype=jnp.float32)
    rising = 10.0 ** (column / D) * jax.random.uniform(first_key, (D,), jnp.float32, 0.6, 1.6)
    values = jnp.clip(jax.random.normal(second_key, (TOK, D), jnp.float32), -4.0, 4.0)
    return jnp.clip(values * rising, -40.0, 40.0).astype(jnp.bfloat16)


def levels(key, extent, shards, least, high):
    loudness, own = 1.0, jax.random.fold_in(key, 6)
    for axis_at, blocks in shards:
        heights = jnp.exp(jax.random.uniform(jax.random.fold_in(own, axis_at), (blocks,), jnp.float32, least / len(shards), high / len(shards)))
        loudness = loudness * jnp.repeat(heights, extent[axis_at] // blocks).reshape([-1 if axis == axis_at else 1 for axis in range(len(extent))])
    return loudness


def centred(key, extent, scale, reach, pieces=(), kind=jnp.bfloat16):
    result = scale * jax.random.normal(key, extent, jnp.float32)
    if pieces:
        result = result * levels(key, extent, pieces, -0.22, 0.18)
    return jnp.clip(result, -reach, reach).astype(kind)


def setup_inputs(seed: int = 0) -> dict:
    keys = jax.random.split(jax.random.key(seed), 17)
    tokens = draw_tokens(jax.random.fold_in(keys[16], 71), 0)
    gain_first = jnp.clip(1.0 + 0.18 * jax.random.normal(keys[1], (D,), jnp.float32), 0.1, 1.9)
    gate_first = centred(keys[2], (D, FF), D ** -0.5, 0.125, ((0, 8), (1, 4)), jnp.float32)
    gate_first_scale = jnp.clip(jnp.exp(math.log(2.0) - 1.3862944 * jax.random.uniform(keys[3], (FF,), jnp.float32) ** levels(keys[3], (FF,), ((0, 4),), -0.2, 0.2)), 0.5, 2.0)
    up_first = centred(keys[4], (D, FF), D ** -0.5, 0.125, ((0, 8), (1, 4)), jnp.float32)
    up_first_scale = jnp.clip(jnp.exp(math.log(2.0) - 1.3862944 * jax.random.uniform(keys[5], (FF,), jnp.float32) ** levels(keys[5], (FF,), ((0, 4),), -0.2, 0.2)), 0.5, 2.0)
    down_first = centred(keys[6], (FF, D), FF ** -0.5, 0.078125, ((0, 4), (1, 8)), jnp.float32)
    down_first_scale = jnp.clip(jnp.exp(jax.random.uniform(keys[7], (D,), jnp.float32, math.log(0.5), math.log(2.0))), 0.5, 2.0)
    gain_second = jnp.clip(1.0 + 0.18 * jax.random.normal(keys[8], (D,), jnp.float32), 0.1, 1.9)
    gate_second = centred(keys[9], (D, FF), D ** -0.5, 0.125, ((0, 8), (1, 4)), jnp.float32)
    gate_second_scale = jnp.clip(jnp.exp(math.log(2.0) - 1.3862944 * jax.random.uniform(keys[10], (FF,), jnp.float32) ** levels(keys[10], (FF,), ((0, 4),), -0.2, 0.2)), 0.5, 2.0)
    up_second = centred(keys[11], (D, FF), D ** -0.5, 0.125, ((0, 8), (1, 4)), jnp.float32)
    up_second_scale = jnp.clip(jnp.exp(math.log(2.0) - 1.3862944 * jax.random.uniform(keys[12], (FF,), jnp.float32) ** levels(keys[12], (FF,), ((0, 4),), -0.2, 0.2)), 0.5, 2.0)
    down_second = centred(keys[13], (FF, D), FF ** -0.5, 0.078125, ((0, 4), (1, 8)), jnp.float32)
    down_second_scale = jnp.clip(jnp.exp(jax.random.uniform(keys[14], (D,), jnp.float32, math.log(0.5), math.log(2.0))), 0.5, 2.0)
    gain_last = jnp.clip(1.0 + 0.18 * jax.random.normal(keys[15], (D,), jnp.float32), 0.1, 1.9)
    return dict(tokens=tokens, gain_first=gain_first, gate_first=gate_first, gate_first_scale=gate_first_scale, up_first=up_first, up_first_scale=up_first_scale, down_first=down_first, down_first_scale=down_first_scale, gain_second=gain_second, gate_second=gate_second, gate_second_scale=gate_second_scale, up_second=up_second, up_second_scale=up_second_scale, down_second=down_second, down_second_scale=down_second_scale, gain_last=gain_last)


def gated_block(values, gain, w_gate, s_gate, w_up, s_up, w_down, s_down):
    meansq = lax.optimization_barrier(jnp.mean(values * values, axis=1, keepdims=True))
    normed = (values * lax.rsqrt(meansq + 1e-06) * gain).astype(jnp.bfloat16)
    gate = jnp.dot(normed, w_gate.astype(jnp.bfloat16), preferred_element_type=jnp.float32) * s_gate
    upper = jnp.dot(normed, w_up.astype(jnp.bfloat16), preferred_element_type=jnp.float32) * s_up
    hidden = (jax.nn.silu(gate) * upper).astype(jnp.bfloat16)
    return jnp.dot(hidden, w_down.astype(jnp.bfloat16), preferred_element_type=jnp.float32) * s_down

def reference(tokens, gain_first, gate_first, gate_first_scale, up_first, up_first_scale, down_first, down_first_scale, gain_second, gate_second, gate_second_scale, up_second, up_second_scale, down_second, down_second_scale, gain_last):
    start = tokens.astype(jnp.float32)
    first = 0.1 * start + 0.5 * gated_block(start, gain_first, gate_first, gate_first_scale, up_first, up_first_scale, down_first, down_first_scale)
    second = 0.1 * first + 0.5 * gated_block(first, gain_second, gate_second, gate_second_scale, up_second, up_second_scale, down_second, down_second_scale)
    meansq = lax.optimization_barrier(jnp.mean(second * second, axis=1, keepdims=True))
    return (second * lax.rsqrt(meansq + 1e-06) * gain_last).astype(jnp.bfloat16)
```

```python
import jax
import jax.numpy as jnp
from jax import lax
from jax.experimental import pallas as pl
from jax.experimental.pallas import tpu as pltpu
from jax.sharding import PartitionSpec as P

D = 2048


def own_slice(vector, width):
    return lax.dynamic_slice_in_dim(vector, lax.axis_index("ra") * width, width, 0)


def full_norm(values, gain):
    meansq = jnp.mean(values * values, axis=1, keepdims=True)
    return (values * lax.rsqrt(meansq + 1e-06) * gain).astype(jnp.bfloat16)


def expand(normed, w_gate, s_gate, w_up, s_up, w_down):
    gate = jnp.dot(
        normed,
        lax.all_gather(w_gate.astype(jnp.bfloat16), "cb", axis=0, tiled=True),
        preferred_element_type=jnp.float32,
    )
    upper = jnp.dot(
        normed,
        lax.all_gather(w_up.astype(jnp.bfloat16), "cb", axis=0, tiled=True),
        preferred_element_type=jnp.float32,
    )
    hidden = (jax.nn.silu(gate * s_gate) * (upper * s_up)).astype(jnp.bfloat16)
    return jnp.dot(
        hidden,
        lax.all_gather(w_down.astype(jnp.bfloat16), "cb", axis=1, tiled=True),
        preferred_element_type=jnp.float32,
    )


def reduce_share(partial_value):
    return lax.psum_scatter(
        partial_value.astype(jnp.bfloat16), "ra", scatter_dimension=1, tiled=True
    ).astype(jnp.float32)


def shards(
    tokens,
    gain_first,
    gate_first,
    gate_first_scale,
    up_first,
    up_first_scale,
    down_first,
    down_first_scale,
    gain_second,
    gate_second,
    gate_second_scale,
    up_second,
    up_second_scale,
    down_second,
    down_second_scale,
    gain_last,
):
    width = tokens.shape[1]
    whole_in = lax.all_gather(tokens, "ra", axis=1, tiled=True).astype(jnp.float32)
    normed = full_norm(whole_in, gain_first)
    partial_value = expand(
        normed, gate_first, gate_first_scale, up_first, up_first_scale, down_first
    )
    summed = lax.psum(partial_value.astype(jnp.bfloat16), "ra").astype(jnp.float32)
    first = 0.1 * whole_in + 0.5 * summed * down_first_scale
    first_share = own_slice(first.T, width).T
    normed_next = full_norm(first, gain_second)
    partial_next = expand(
        normed_next, gate_second, gate_second_scale, up_second, up_second_scale, down_second
    )
    second = 0.1 * first_share + 0.5 * reduce_share(partial_next) * own_slice(
        down_second_scale, width
    )
    closing = lax.psum(jnp.sum(second * second, axis=1), "ra")
    return (second * lax.rsqrt(closing / D + 1e-06)[:, None] * own_slice(gain_last, width)).astype(
        jnp.bfloat16
    )


def cast(values):
    return values.astype(jnp.bfloat16)


def swap(values, axis, mask):
    size = lax.axis_size(axis)
    return lax.ppermute(values, axis, [(i, i ^ mask) for i in range(size)])


def assemble(pieces, orders):
    count = sum(p.shape[0] for p in pieces[0])
    _, half, width = pieces[0][0].shape
    sizes = [[p.shape[0] for p in side] for side in pieces]

    def kernel(*refs):
        *sources, out = refs
        sources = iter(sources)
        for side, (order, lengths) in enumerate(zip(orders, sizes)):
            at = 0
            for length in lengths:
                source = next(sources)
                for i in range(length):
                    j = order[at + i]
                    out[side * half : (side + 1) * half, j * width : (j + 1) * width] = source[i]
                at += length

    flat = [p for side in pieces for p in side]
    return pl.pallas_call(
        kernel,
        out_shape=jax.ShapeDtypeStruct((2 * half, count * width), flat[0].dtype),
        in_specs=[pl.BlockSpec(memory_space=pltpu.VMEM)] * len(flat),
        out_specs=pl.BlockSpec(memory_space=pltpu.VMEM),
        compiler_params=pltpu.CompilerParams(vmem_limit_bytes=5 * half * count * width * 4),
        cost_estimate=pl.CostEstimate(
            flops=8 * half * count * width,
            bytes_accessed=8 * half * count * width,
            transcendentals=0,
        ),
    )(*flat)


def gather_ra(block):
    half = block.shape[0] // 2
    top, low = [block[None, :half]], [block[None, half:]]
    bits = [1 << b for b in range(lax.axis_size("ra").bit_length() - 1)]
    top_order, low_order = [0], [0]
    for up_bit, down_bit in zip(bits, reversed(bits)):
        top_new = swap(top[0] if len(top) == 1 else jnp.concatenate(top), "ra", up_bit)
        low_new = swap(low[0] if len(low) == 1 else jnp.concatenate(low), "ra", down_bit)
        top_order += [j ^ up_bit for j in top_order]
        low_order += [j ^ down_bit for j in low_order]
        top.append(top_new)
        low.append(low_new)
    return assemble([top, low], [top_order, low_order])


def reduce_ra(values, width):
    half = values.shape[0] // 2
    count = lax.axis_size("ra")
    bits = [1 << b for b in range(count.bit_length() - 1)]
    top = {j: values[:half, j * width : (j + 1) * width] for j in range(count)}
    low = {j: values[half:, j * width : (j + 1) * width] for j in range(count)}

    def halve(parts, bit):
        keep = [j for j in parts if not j & bit]
        sent = jnp.stack([cast(parts[j ^ bit]) for j in keep])
        got = swap(sent, "ra", bit)
        return {
            j: parts[j].astype(jnp.float32) + got[at].astype(jnp.float32)
            for at, j in enumerate(keep)
        }

    for up_bit, down_bit in zip(bits, reversed(bits)):
        top = halve(top, down_bit)
        low = halve(low, up_bit)
    return jnp.concatenate([top[0], low[0]], axis=0)


def sum_ra(values):
    count = lax.axis_size("ra")
    for b in range(count.bit_length() - 1):
        values = values + swap(values, "ra", 1 << b)
    return values


def relative(blocks):
    me = lax.axis_index("ra")
    return [
        lax.dynamic_index_in_dim(blocks, me ^ j, 0, keepdims=False)
        for j in range(blocks.shape[0])
    ]


def lanes():
    size = lax.axis_size("cb")
    return [list(range(core, size, 2)) for core in range(2)]


def exchange(chunks):
    got = lax.all_to_all(chunks, "cb", 0, 0, axis_index_groups=lanes())
    other = swap(got, "cb", 1)
    south = lax.rem(lax.axis_index("cb"), 2) == 0
    return jnp.stack([jnp.where(south, got, other), jnp.where(south, other, got)], axis=1)


def reshard(weights):
    rows, columns = weights[0].shape
    chips = lax.axis_size("cb") // 2
    chunks = jnp.stack(
        [cast(w).reshape(rows, chips, columns // chips).transpose(1, 0, 2) for w in weights],
        axis=1,
    )
    whole = exchange(chunks)
    whole = whole.reshape(lax.axis_size("ra"), -1, *chunks.shape[1:])
    parts = relative(whole)
    return [
        jnp.concatenate([piece[at] for part in parts for piece in part], axis=0)
        for at in range(len(weights))
    ]


def hidden_slice(scale):
    size = scale.shape[0] // (lax.axis_size("cb") // 2)
    return lax.dynamic_slice_in_dim(scale, lax.axis_index("cb") // 2 * size, size, 0)


def groups_of(chips):
    return [[0], list(range(1, chips))]


def row_norm(values, gain):
    meansq = sum_ra(jnp.sum(values * values, axis=1)) / D
    return values * lax.rsqrt(meansq + 1e-06)[:, None] * own_slice(gain, values.shape[1])


def hidden_groups(own, w_gate, s_gate, w_up, s_up):
    chips = lax.axis_size("cb") // 2
    half = own.shape[0] // 2
    s_gate, s_up = hidden_slice(s_gate), hidden_slice(s_up)
    arrived = [own] + [swap(own, "cb", 2 * k) for k in range(1, chips)]
    results = []
    for members in groups_of(chips):
        stacked = [arrived[k] for k in members]
        block = jnp.concatenate(
            [s[:half] for s in stacked] + [s[half:] for s in stacked], axis=0
        )
        normed = gather_ra(block)
        gate = jnp.dot(normed, w_gate, preferred_element_type=jnp.float32)
        upper = jnp.dot(normed, w_up, preferred_element_type=jnp.float32)
        results.append(cast(jax.nn.silu(gate * s_gate) * (upper * s_up)))
    return results


def summed_down(hiddens, w_down, shape):
    rows, width = shape
    chips = lax.axis_size("cb") // 2
    total = None
    for members, hidden in reversed(list(zip(groups_of(chips), hiddens))):
        product = lax.dot_general(
            hidden, w_down, (((1,), (1,)), ((), ())), preferred_element_type=jnp.float32
        )
        summed = reduce_ra(cast(product), width)
        summed = summed.reshape(2, len(members), rows // 2, width)
        for at, k in enumerate(members):
            part = summed[:, at].reshape(rows, width)
            if k:
                part = swap(cast(part), "cb", 2 * k).astype(jnp.float32)
            total = part if total is None else total + part
    return total


def resharded(
    tokens,
    gain_first,
    gate_first,
    gate_first_scale,
    up_first,
    up_first_scale,
    down_first,
    down_first_scale,
    gain_second,
    gate_second,
    gate_second_scale,
    up_second,
    up_second_scale,
    down_second,
    down_second_scale,
    gain_last,
):
    shape = tokens.shape
    width = shape[1]
    start = tokens.astype(jnp.float32)
    w_gate, w_up = reshard([gate_first, up_first])
    w_gate, gate_second, up_second, down_second = lax.optimization_barrier(
        (w_gate, gate_second, up_second, down_second)
    )
    (w_down,) = reshard([down_first.T])
    hiddens = hidden_groups(
        cast(row_norm(start, gain_first)), w_gate, gate_first_scale, w_up, up_first_scale
    )
    w_gate, w_up, w_down_second = reshard([gate_second, up_second, down_second.T])
    b_first = summed_down(hiddens, w_down, shape)
    first = 0.1 * start + 0.5 * b_first * own_slice(down_first_scale, width)
    hiddens = hidden_groups(
        cast(row_norm(first, gain_second)), w_gate, gate_second_scale, w_up, up_second_scale
    )
    second = 0.1 * first + 0.5 * summed_down(hiddens, w_down_second, shape) * own_slice(
        down_second_scale, width
    )
    return cast(row_norm(second, gain_last))


def plan_for(mesh):
    ra, cb = mesh.shape["ra"], mesh.shape["cb"]

    def run(tokens, *rest):
        weight = rest[1]
        activations = 4 * tokens.size * ra * cb // 2
        weights = 6 * weight.size * cb
        regular = cb % 2 == 0 and not (cb // 2) & (cb // 2 - 1) and not ra & (ra - 1)
        if regular and activations < weights:
            return resharded(tokens, *rest)
        return shards(tokens, *rest)

    return run


def solution(mesh):
    placed = (
        P("cb", "ra"),
        P(),
        P("cb", "ra"),
        P("ra"),
        P("cb", "ra"),
        P("ra"),
        P("ra", "cb"),
        P(),
        P(),
        P("cb", "ra"),
        P("ra"),
        P("cb", "ra"),
        P("ra"),
        P("ra", "cb"),
        P(),
        P(),
    )
    return jax.shard_map(
        plan_for(mesh), mesh=mesh, in_specs=placed, out_specs=P("cb", "ra"), check_vma=False
    )
```
